32 devices in a mesh: sp: 8 (over z, x), dp: 4 (over y, core).
Axes of the slice: x: 2, y: 2, z: 4, core: 2. Of those that a mesh axis runs over, the one named last changes fastest.
Arguments:
- skip_stream_entering: bfloat16 [4, 1024, 2048], P('dp', 'sp'), may hold values from -6 to 6
- mapped_probe_matrix: bfloat16 [4, 1024, 2048], P('dp', 'sp'), may hold values from -6 to 6
- mapped_lookup_matrix: bfloat16 [4, 1024, 2048], P('dp', 'sp'), may hold values from -6 to 6
- mapped_content_matrix: bfloat16 [4, 1024, 4096], P('dp', 'sp'), may hold values from -6 to 6
- retention_preactivation: bfloat16 [4, 1024, 2048], P('dp', 'sp'), may hold values from -4 to 12
- extra_shrinkage: float32 [4, 16, 1024], P('dp', 'sp'), may hold values from -0.6932 to 0
- attention_group_scale: float32 [4096], replicated, may hold values from 0.1 to 1.9
- final_projection_matrix: bfloat16 [4096, 2048], P(None, 'dp'), may hold values from -0.09375 to 0.09375
- blender_branch_scale: float32 [2048], replicated, may hold values from 0.1 to 1.9
- specialist_prenormal_scale: float32 [2048], replicated, may hold values from 0.1 to 1.9
- specialist_switch_matrix: bfloat16 [32, 2048, 1024], P(('sp', 'dp')), may hold values from -0.125 to 0.125
- specialist_expand_matrix: bfloat16 [32, 2048, 1024], P(('sp', 'dp')), may hold values from -0.125 to 0.125
- specialist_contract_matrix: bfloat16 [32, 1024, 2048], P(('sp', 'dp')), may hold values from -0.1875 to 0.1875
- specialist_branch_scale: float32 [2048], replicated, may hold values from 0.1 to 1.9
- assigned_specialists: int32 [4, 1024, 2], P('dp', 'sp'), may hold values from 0 to 31, all different within a row; in each aligned block of 128 rows (0 to 127, 128 to 255, ..., all dimensions but the last counted through in order) at most 13 rows name the same one
- dispatcher_logits: float32 [4, 1024, 2], P('dp', 'sp'), may hold values from 0.2 to 1
Outputs:
- layer_out: bfloat16 [4, 1024, 2048], P('dp', 'sp')
The draws below stay inside these ranges and needn't reach their ends.
Inputs may be any that keep to these rules, and one draw needn't show every extreme that they name: `assigned_specialists`: in the rows of one device no expert is named more than 13 times; in every draw some expert reaches 13 on some device.
All inputs are finite; a program needn't handle non-finite values.
Results may differ from the reference program's by a relative error of at most 0.013.
Values may be sent and summed in bfloat16 or wider, within the bound.
A program may use at most 128 MiB of HBM per device.

```python
import math
import jax
import jax.numpy as jnp
import numpy as np
from jax import lax

D = 2048
ATTENTION_GROUPS = 16
KEY_WIDTH = 128
DV = 256
FF = 1024
TOP = 2
BLOCK = 64
TOK_DEV = 128
BATCH_SAMPLES = 4
TIME_STEPS = 1024
EXPERTS = 32
CAP = 13


def draw_retention_preactivation(key, part):
    kinds = jax.random.randint(jax.random.fold_in(key, 11), (ATTENTION_GROUPS,), 0, 10)
    slowness = (kinds >= 5).astype(jnp.float32)
    slow_center = math.log(TIME_STEPS / 24.0)
    centers = slowness * slow_center + (1.0 - slowness) * 0.5
    channel = jax.random.uniform(jax.random.fold_in(key, 12), (ATTENTION_GROUPS, KEY_WIDTH), jnp.float32, -0.5, 0.5)
    base_rate = (centers[:, None] + channel).reshape(ATTENTION_GROUPS * KEY_WIDTH)
    span_count = TIME_STEPS // TOK_DEV
    shifts = jax.random.uniform(jax.random.fold_in(key, 13), (BATCH_SAMPLES, span_count), jnp.float32, -0.7, 0.7)
    shifts = jnp.repeat(shifts, TOK_DEV, axis=1)
    jitter = 0.8 * jax.random.normal(jax.random.fold_in(key, 14), (BATCH_SAMPLES, TIME_STEPS, ATTENTION_GROUPS * KEY_WIDTH), jnp.float32)
    total = base_rate[None, None, :] + shifts[:, :, None] + jitter
    return jnp.clip(total, -4.0, 12.0).astype(jnp.bfloat16)


def draw_extra_shrinkage(key, part):
    spike_amount = 6
    timestep_offset = jax.random.randint(jax.random.fold_in(key, 21), (BATCH_SAMPLES, ATTENTION_GROUPS, spike_amount), 0, TIME_STEPS)
    tier_amount = jax.random.uniform(jax.random.fold_in(key, 22), (BATCH_SAMPLES, ATTENTION_GROUPS, spike_amount), jnp.float32, math.log(0.5), math.log(0.8))
    places = jnp.arange(TIME_STEPS, dtype=jnp.int32)
    matched = places[None, None, :, None] == timestep_offset[:, :, None, :]
    return jnp.min(jnp.where(matched, tier_amount[:, :, None, :], 0.0), axis=3)


def block_scale(key, dims, split, low, high):
    level = 1.0
    for dim, blocks in split:
        draws = jax.random.uniform(jax.random.fold_in(jax.random.fold_in(key, 6), dim), (blocks,), jnp.float32, low / len(split), high / len(split))
        level = level * jnp.repeat(jnp.exp(draws), dims[dim] // blocks).reshape((-1,) + (1,) * (len(dims) - 1 - dim))
    return level


def assign_block(stream_key, own, number, rows, number_of, top, bound, skew):
    order = jax.random.permutation(stream_key, number_of)
    packed, common = portions_of(number_of, rows * top, bound, skew, True), portions_of(number_of, rows * top, bound, skew, False)
    places = jnp.arange(number_of)

    def named(lengths, rotation):
        used = int((lengths > 0).sum())
        fixed = max(1, used // 4)
        shifted = fixed + (places - fixed + rotation * (used - fixed)) % max(1, number_of - fixed)
        return jnp.zeros((number_of,), jnp.int32).at[order[jnp.where(places < fixed, places, shifted)]].set(jnp.asarray(lengths, jnp.int32))

    lengths = jnp.where(number % 4 == 0, named(packed, number // 4), named(common, number - number // 4 - 1))
    mixed = jax.random.permutation(jax.random.fold_in(own, 3), number_of)
    donor, taker = mixed[0:number_of // 2 * 2:2], mixed[1:number_of // 2 * 2:2]
    room = jnp.minimum(lengths[donor] - 1, bound - lengths[taker]) // 2
    room = jnp.where((donor == order[0]) | (taker == order[0]) | (lengths[taker] == 0), 0, jnp.maximum(room, 0))
    shifted = jax.random.randint(jax.random.fold_in(own, 4), (number_of // 2,), 0, 1 << 20) % (room + 1)
    lengths = lengths.at[donor].add(-shifted).at[taker].add(shifted)
    members = jnp.searchsorted(jnp.cumsum(lengths), jnp.arange(rows * top), side="right").astype(jnp.int32)
    listing = members.reshape(top, rows).T
    listing = listing[jax.random.permutation(jax.random.fold_in(own, 1), rows)]
    rotation = jax.random.randint(jax.random.fold_in(own, 2), (rows, 1), 0, top)
    return jnp.take_along_axis(listing, (jnp.arange(top)[None, :] + rotation) % top, axis=1)


def portions_of(amount, total, bound, slope, full):
    weights = [(1 << 20) // math.isqrt(rank ** slope) + 1 for rank in range(1, amount + 1)]
    largest = bound if full else min(bound, max(-(-total // amount), total * weights[0] // sum(weights)))
    least = 1 if total - largest >= amount - 1 else 0
    holding, surplus = [largest] + [least] * (amount - 1), total - largest - least * (amount - 1)
    while surplus > 0:
        free = [i for i in range(1, amount) if holding[i] < largest] or [i for i in range(1, amount) if holding[i] < bound]
        whole, budget = sum([weights[i] for i in free]), surplus
        for i in free:
            extra = min(bound - holding[i], max(1, budget * weights[i] // whole), surplus)
            holding[i] = holding[i] + extra
            surplus = surplus - extra
    return np.array(holding)


def centred(own_key, shape, scale, limit, split=(), kind=jnp.bfloat16):
    drawn = jax.random.normal(own_key, shape, jnp.float32) * scale
    if len(split) > 0:
        drawn = block_scale(own_key, shape, split, -0.22, 0.18) * drawn
    return jnp.clip(drawn, min=-limit, max=limit).astype(kind)


def setup_inputs(seed: int = 0) -> dict:
    key_list = jax.random.split(jax.random.key(seed), 17)
    skip_stream_entering = centred(key_list[0], (BATCH_SAMPLES, TIME_STEPS, D), 1.0, 6.0, ((0, 4), (1, 8)))
    mapped_probe_matrix = centred(key_list[1], (BATCH_SAMPLES, TIME_STEPS, ATTENTION_GROUPS * KEY_WIDTH), 1.0, 6.0, ((0, 4), (1, 8)))
    mapped_lookup_matrix = centred(key_list[2], (BATCH_SAMPLES, TIME_STEPS, ATTENTION_GROUPS * KEY_WIDTH), 1.0, 6.0, ((0, 4), (1, 8)))
    mapped_content_matrix = centred(key_list[3], (BATCH_SAMPLES, TIME_STEPS, ATTENTION_GROUPS * DV), 1.0, 6.0, ((0, 4), (1, 8)))
    retention_preactivation = draw_retention_preactivation(jax.random.fold_in(key_list[16], 71), 0)
    extra_shrinkage = draw_extra_shrinkage(jax.random.fold_in(key_list[16], 71), 0)
    attention_group_scale = jnp.clip(1.0 + 0.18 * jax.random.normal(key_list[6], (ATTENTION_GROUPS * DV,), jnp.float32), 0.1, 1.9)
    final_projection_matrix = centred(key_list[7], (ATTENTION_GROUPS * DV, D), (ATTENTION_GROUPS * DV) ** -0.5, 0.09375, ((1, 4),))
    blender_branch_scale = jnp.clip(1.0 + 0.18 * jax.random.normal(key_list[8], (D,), jnp.float32), 0.1, 1.9)
    specialist_prenormal_scale = jnp.clip(1.0 + 0.18 * jax.random.normal(key_list[9], (D,), jnp.float32), 0.1, 1.9)
    specialist_switch_matrix = centred(key_list[10], (EXPERTS, D, FF), D ** -0.5, 0.125, ((0, 32),))
    specialist_expand_matrix = centred(key_list[11], (EXPERTS, D, FF), D ** -0.5, 0.125, ((0, 32),))
    specialist_contract_matrix = centred(key_list[12], (EXPERTS, FF, D), FF ** -0.5, 0.1875, ((0, 32),))
    specialist_branch_scale = jnp.clip(1.0 + 0.18 * jax.random.normal(key_list[13], (D,), jnp.float32), 0.1, 1.9)
    assigned_specialists_keys = jax.random.split(jax.random.fold_in(key_list[14], 1), BATCH_SAMPLES * TIME_STEPS // TOK_DEV)
    assigned_specialists_turns = jax.random.permutation(jax.random.fold_in(key_list[14], 3), BATCH_SAMPLES * TIME_STEPS // TOK_DEV)
    assigned_specialists = jax.vmap(lambda own, number: assign_block(jax.random.fold_in(key_list[14], 2), own, number, TOK_DEV, EXPERTS, TOP, CAP, 2))(assigned_specialists_keys, assigned_specialists_turns).reshape((BATCH_SAMPLES, TIME_STEPS, TOP))
    dispatcher_logits = jnp.clip(jnp.exp(math.log(1.0) - 1.609438 * jax.random.uniform(key_list[15], (BATCH_SAMPLES, TIME_STEPS, TOP), jnp.float32) ** block_scale(key_list[15], (BATCH_SAMPLES, TIME_STEPS, TOP), ((0, 4), (1, 8)), -0.2, 0.2)), 0.2, 1.0)
    return dict(skip_stream_entering=skip_stream_entering, mapped_probe_matrix=mapped_probe_matrix, mapped_lookup_matrix=mapped_lookup_matrix, mapped_content_matrix=mapped_content_matrix, retention_preactivation=retention_preactivation, extra_shrinkage=extra_shrinkage, attention_group_scale=attention_group_scale, final_projection_matrix=final_projection_matrix, blender_branch_scale=blender_branch_scale, specialist_prenormal_scale=specialist_prenormal_scale, specialist_switch_matrix=specialist_switch_matrix, specialist_expand_matrix=specialist_expand_matrix, specialist_contract_matrix=specialist_contract_matrix, specialist_branch_scale=specialist_branch_scale, assigned_specialists=assigned_specialists, dispatcher_logits=dispatcher_logits)


epsilon = 1e-06
softness_factor = 16.0
highest = lax.Precision.HIGHEST

def rms_scale(values, gain):
    mean_square = lax.optimization_barrier(jnp.mean(values * values, axis=-1, keepdims=True))
    return values * lax.rsqrt(mean_square + epsilon) * gain

def combine_states(earlier, later):
    return (earlier[0] * later[0], later[0][..., None] * earlier[1] + later[1])

def block_attention(query_f, key_f, value_f, shrink_exponent):
    length_value, head_count, key_dim = query_f.shape
    value_dim = value_f.shape[-1]
    block_count = length_value // BLOCK
    query_blocks = query_f.reshape(block_count, BLOCK, head_count, key_dim)
    key_blocks = key_f.reshape(block_count, BLOCK, head_count, key_dim)
    value_blocks = value_f.reshape(block_count, BLOCK, head_count, value_dim)
    within = jnp.cumsum(shrink_exponent.reshape(block_count, BLOCK, head_count, key_dim), axis=1)
    block_end = within[:, -1]
    lifted = query_blocks * jnp.exp(within)
    lowered = key_blocks * jnp.exp(-within)
    scores = jnp.einsum('nthk,nshk->nhts', lifted, lowered, precision=highest)
    causal = jnp.arange(BLOCK)[:, None] >= jnp.arange(BLOCK)[None, :]
    scores = jnp.where(causal, scores, 0.0)
    inside = jnp.einsum('nhts,nshv->nthv', scores, value_blocks, precision=highest)
    carried_keys = key_blocks * jnp.exp(block_end[:, None] - within)
    updates = jnp.einsum('nshk,nshv->nhkv', carried_keys, value_blocks, precision=highest)
    decays = jnp.exp(block_end)
    total_decay, states = lax.associative_scan(combine_states, (decays, updates), axis=0)
    entering = jnp.concatenate([jnp.zeros_like(states[:1]), states[:-1]], axis=0)
    across = jnp.einsum('nthk,nhkv->nthv', lifted, entering, precision=highest)
    outputs = (inside + across).reshape(length_value, head_count, value_dim)
    offsets = jnp.cumsum(block_end, axis=0) - block_end
    reached = (query_blocks * jnp.exp(within + offsets[:, None])).reshape(length_value, head_count, key_dim)
    return (outputs, total_decay[-1], states[-1], reached)

def reference(skip_stream_entering, mapped_probe_matrix, mapped_lookup_matrix, mapped_content_matrix, retention_preactivation, extra_shrinkage, attention_group_scale, final_projection_matrix, blender_branch_scale, specialist_prenormal_scale, specialist_switch_matrix, specialist_expand_matrix, specialist_contract_matrix, specialist_branch_scale, assigned_specialists, dispatcher_logits):

    def lone_series(fragment_array):
        probe_series, lookup_series, content_series, shrink_series, spike_series = fragment_array
        length_value = probe_series.shape[0]
        query_f = probe_series.reshape(length_value, ATTENTION_GROUPS, KEY_WIDTH).astype(jnp.float32) * KEY_WIDTH ** (-0.5)
        key_f = lookup_series.reshape(length_value, ATTENTION_GROUPS, KEY_WIDTH).astype(jnp.float32)
        value_f = content_series.reshape(length_value, ATTENTION_GROUPS, DV).astype(jnp.float32)
        shrink_exponent = jax.nn.log_sigmoid(shrink_series.reshape(length_value, ATTENTION_GROUPS, KEY_WIDTH).astype(jnp.float32)) / softness_factor
        shrink_exponent = shrink_exponent + jnp.transpose(spike_series)[:, :, None]
        outputs = block_attention(query_f, key_f, value_f, shrink_exponent)[0]
        return rms_scale(outputs, attention_group_scale.reshape(ATTENTION_GROUPS, DV)).astype(jnp.bfloat16)
    attention_group_result = lax.map(lone_series, (mapped_probe_matrix, mapped_lookup_matrix, mapped_content_matrix, retention_preactivation, extra_shrinkage))
    token_count = BATCH_SAMPLES * TIME_STEPS
    attention_group_result = attention_group_result.reshape(token_count, ATTENTION_GROUPS * DV)
    projected = jnp.dot(attention_group_result, final_projection_matrix, preferred_element_type=jnp.float32).astype(jnp.bfloat16)
    stream = skip_stream_entering.reshape(token_count, D).astype(jnp.float32)
    residual = (stream + rms_scale(projected.astype(jnp.float32), blender_branch_scale)).astype(jnp.bfloat16)
    expert_in = rms_scale(residual.astype(jnp.float32), specialist_prenormal_scale).astype(jnp.bfloat16)
    block_total = token_count // TOK_DEV
    pair_dev = TOK_DEV * TOP
    pair_count = token_count * TOP
    chosen = assigned_specialists.reshape(block_total, pair_dev)
    onehot = (chosen[:, :, None] == jnp.arange(EXPERTS, dtype=jnp.int32)[None, None, :]).astype(jnp.int32)
    ranks = lax.optimization_barrier(jnp.sum((jnp.cumsum(onehot, axis=1) - onehot) * onehot, axis=2))
    block_ids = jnp.arange(block_total, dtype=jnp.int32)[:, None]
    slots = (chosen * block_total + block_ids) * CAP + ranks
    pair_ids = jnp.arange(pair_count, dtype=jnp.int32)
    table = jnp.full((EXPERTS * block_total * CAP,), pair_count, jnp.int32)
    table = table.at[slots.reshape(-1)].set(pair_ids).reshape(EXPERTS, block_total * CAP)
    padded = jnp.concatenate([expert_in, jnp.zeros((1, D), jnp.bfloat16)], axis=0)

    def expert_step(carry, fragment_array):
        sources, gate_weight, up_weight, down_weight = fragment_array
        row_block = padded[sources // TOP]
        gate_part = jnp.dot(row_block, gate_weight, preferred_element_type=jnp.float32)
        up_part = jnp.dot(row_block, up_weight, preferred_element_type=jnp.float32)
        hidden_units = (jax.nn.silu(gate_part) * up_part).astype(jnp.bfloat16)
        result = jnp.dot(hidden_units, down_weight, preferred_element_type=jnp.float32).astype(jnp.bfloat16)
        return (carry.at[sources].set(result, mode='drop'), None)
    pair_out, _ = lax.scan(expert_step, jnp.zeros((pair_count, D), jnp.bfloat16), (table, specialist_switch_matrix, specialist_expand_matrix, specialist_contract_matrix))
    weights = dispatcher_logits.reshape(token_count, TOP)
    weights = weights / lax.optimization_barrier(jnp.sum(weights, axis=1, keepdims=True))
    combined = lax.optimization_barrier(jnp.sum(pair_out.reshape(token_count, TOP, D).astype(jnp.float32) * weights[:, :, None], axis=1))
    layer_out = residual.astype(jnp.float32) + rms_scale(combined, specialist_branch_scale)
    return layer_out.astype(jnp.bfloat16).reshape(BATCH_SAMPLES, TIME_STEPS, D)
```

```python
import jax
import jax.numpy as jnp
from jax import lax
from jax.experimental import pallas as pl
from jax.experimental.pallas import tpu as pltpu
from jax.sharding import PartitionSpec as P

D = 2048
KEY_WIDTH = 128
DV = 256
TOP = 2
BLOCK = 64


epsilon = 1e-06
softness_factor = 16.0
highest = lax.Precision.HIGHEST


def rms_scale(values, gain):
    mean_square = jnp.mean(values * values, axis=-1, keepdims=True)
    return values * lax.rsqrt(mean_square + epsilon) * gain


def local_kernel(q_ref, k_ref, v_ref, g_ref, e_ref, o_ref, r_ref, u_ref):
    rows = q_ref.shape[0]
    g = g_ref[...].astype(jnp.float32)
    logs = (jnp.minimum(g, 0.0) - jnp.log(1.0 + jnp.exp(-jnp.abs(g)))) / softness_factor
    row = lax.broadcasted_iota(jnp.int32, (rows, rows), 0)
    col = lax.broadcasted_iota(jnp.int32, (rows, rows), 1)
    causal = row >= col
    extra = jnp.sum(jnp.where(causal, e_ref[0], 0.0), axis=1, keepdims=True)
    within = extra + jnp.dot(
        causal.astype(jnp.float32), logs, precision=highest, preferred_element_type=jnp.float32
    )
    middle = within[rows // 2 - 1 : rows // 2]
    end = within[rows - 1 : rows]
    q = q_ref[...].astype(jnp.float32) * KEY_WIDTH ** (-0.5)
    k = k_ref[...].astype(jnp.float32)
    v = v_ref[...]
    lifted = (q * jnp.exp(within - middle)).astype(jnp.bfloat16)
    lowered = (k * jnp.exp(middle - within)).astype(jnp.bfloat16)
    scores = lax.dot_general(
        lifted, lowered, (((1,), (1,)), ((), ())), preferred_element_type=jnp.float32
    )
    scores = jnp.where(causal, scores, 0.0).astype(jnp.bfloat16)
    o_ref[...] = jnp.dot(scores, v, preferred_element_type=jnp.float32)
    r_ref[...] = (q * jnp.exp(within)).astype(jnp.bfloat16)
    carried = (k * jnp.exp(end - within)).astype(jnp.bfloat16)
    u_ref[0] = lax.dot_general(
        v, carried, (((0,), (0,)), ((), ())), preferred_element_type=jnp.float32
    ).astype(jnp.bfloat16)


def scan_kernel(u_ref, d_ref, s_ref):
    count = u_ref.shape[0]
    decay = jnp.exp(d_ref[0])
    state = jnp.zeros(u_ref.shape[2:], jnp.float32)
    for i in range(count):
        s_ref[i, 0] = state.astype(jnp.bfloat16)
        if i < count - 1:
            state = state * decay[i : i + 1] + u_ref[i, 0].astype(jnp.float32)


def finish_kernel(o_ref, r_ref, s_ref, gain_ref, out_ref):
    mixed = o_ref[...] + lax.dot_general(
        r_ref[...], s_ref[0], (((1,), (1,)), ((), ())), preferred_element_type=jnp.float32
    )
    out_ref[...] = rms_scale(mixed, gain_ref[...]).astype(jnp.bfloat16)


def linear_attention(query, key, value, gate, extra_shrinkage, gains):
    rows, width = query.shape
    heads = width // KEY_WIDTH
    sp_count = lax.axis_size("sp")
    own = extra_shrinkage.shape[0]
    logs = jnp.sum(jax.nn.log_sigmoid(gate.astype(jnp.float32)), axis=0) / softness_factor
    spans = jnp.transpose(extra_shrinkage.reshape(own, sp_count, rows), (1, 0, 2))
    small = jnp.concatenate([spans, logs.reshape(sp_count, own, KEY_WIDTH)], axis=2)
    small = lax.all_to_all(small, "sp", split_axis=0, concat_axis=0, tiled=True)
    extra = small[:, :, :rows].reshape(heads, 1, rows)
    decays = jnp.transpose(small[:, :, rows:] + jnp.sum(spans, axis=2)[:, :, None], (1, 0, 2))
    narrow = pl.BlockSpec((rows, KEY_WIDTH), lambda h: (0, h))
    wide = pl.BlockSpec((rows, DV), lambda h: (0, h))
    state = pl.BlockSpec((1, DV, KEY_WIDTH), lambda h: (h, 0, 0))
    inside, reached, updates = pl.pallas_call(
        local_kernel,
        grid=(heads,),
        in_specs=[narrow, narrow, wide, narrow, pl.BlockSpec((1, 1, rows), lambda h: (h, 0, 0))],
        out_specs=[wide, narrow, state],
        out_shape=[
            jax.ShapeDtypeStruct((rows, heads * DV), jnp.float32),
            jax.ShapeDtypeStruct((rows, width), jnp.bfloat16),
            jax.ShapeDtypeStruct((heads, DV, KEY_WIDTH), jnp.bfloat16),
        ],
        name="local",
    )(query, key, value, gate, extra)
    gathered = lax.all_to_all(updates, "sp", split_axis=0, concat_axis=0, tiled=True)
    stack = pl.BlockSpec((sp_count, 1, DV, KEY_WIDTH), lambda h: (0, h, 0, 0))
    entering = pl.pallas_call(
        scan_kernel,
        grid=(own,),
        in_specs=[stack, pl.BlockSpec((1, sp_count, KEY_WIDTH), lambda h: (h, 0, 0))],
        out_specs=stack,
        out_shape=jax.ShapeDtypeStruct((sp_count, own, DV, KEY_WIDTH), jnp.bfloat16),
        name="scan",
    )(gathered.reshape(sp_count, own, DV, KEY_WIDTH), decays)
    entering = lax.all_to_all(
        entering.reshape(updates.shape), "sp", split_axis=0, concat_axis=0, tiled=True
    )
    return pl.pallas_call(
        finish_kernel,
        grid=(heads,),
        in_specs=[wide, narrow, state, pl.BlockSpec((1, DV), lambda h: (0, h))],
        out_specs=wide,
        out_shape=jax.ShapeDtypeStruct((rows, heads * DV), jnp.bfloat16),
        name="finish",
    )(inside, reached, entering, gains.reshape(1, heads * DV))


def shards(
    skip_stream_entering,
    mapped_probe_matrix,
    mapped_lookup_matrix,
    mapped_content_matrix,
    retention_preactivation,
    extra_shrinkage,
    attention_group_scale,
    final_projection_matrix,
    blender_branch_scale,
    specialist_prenormal_scale,
    specialist_switch_matrix,
    specialist_expand_matrix,
    specialist_contract_matrix,
    specialist_branch_scale,
    assigned_specialists,
    dispatcher_logits,
):
    tok_rows = mapped_probe_matrix.shape[1]
    sp_count = lax.axis_size("sp")
    dp_count = lax.axis_size("dp")
    flat_heads = linear_attention(
        mapped_probe_matrix[0],
        mapped_lookup_matrix[0],
        mapped_content_matrix[0],
        retention_preactivation[0],
        extra_shrinkage[0],
        attention_group_scale,
    )
    projected = jnp.dot(
        flat_heads,
        lax.all_gather(final_projection_matrix, "dp", axis=1, tiled=True),
        preferred_element_type=jnp.float32,
    ).astype(jnp.bfloat16)
    stream = skip_stream_entering[0].astype(jnp.float32)
    residual = (stream + rms_scale(projected.astype(jnp.float32), blender_branch_scale)).astype(
        jnp.bfloat16
    )
    expert_in = rms_scale(residual.astype(jnp.float32), specialist_prenormal_scale).astype(
        jnp.bfloat16
    )
    expert_total = sp_count * dp_count
    capacity = max(2, 5 * tok_rows * TOP // (3 * expert_total))
    chosen = assigned_specialists[0].reshape(-1)
    pair_total = chosen.shape[0]
    onehot = (chosen[:, None] == jnp.arange(expert_total, dtype=jnp.int32)[None, :]).astype(
        jnp.int32
    )
    ranks = jnp.sum((jnp.cumsum(onehot, axis=0) - onehot) * onehot, axis=1)
    slots = chosen * capacity + ranks
    table = jnp.full((expert_total * capacity,), pair_total, jnp.int32)
    table = table.at[slots].set(jnp.arange(pair_total, dtype=jnp.int32))
    padded = jnp.concatenate([expert_in, jnp.zeros((1, D), jnp.bfloat16)], axis=0)
    outgoing = padded[table // TOP].reshape(expert_total, capacity, D)
    arrived_rows = lax.all_to_all(outgoing, ("sp", "dp"), split_axis=0, concat_axis=0, tiled=True)
    row_block = arrived_rows.reshape(-1, D)
    gate_part = jnp.dot(row_block, specialist_switch_matrix[0], preferred_element_type=jnp.float32)
    up_part = jnp.dot(row_block, specialist_expand_matrix[0], preferred_element_type=jnp.float32)
    hidden_units = (jax.nn.silu(gate_part) * up_part).astype(jnp.bfloat16)
    result = jnp.dot(
        hidden_units, specialist_contract_matrix[0], preferred_element_type=jnp.float32
    )
    returned = lax.all_to_all(
        result.astype(jnp.bfloat16).reshape(arrived_rows.shape),
        ("sp", "dp"),
        split_axis=0,
        concat_axis=0,
        tiled=True,
    )
    flat_back = returned.reshape(expert_total * capacity, D)
    pair_rows = flat_back[slots].reshape(tok_rows, TOP, D)
    weights = dispatcher_logits[0]
    weights = weights / jnp.sum(weights, axis=1, keepdims=True)
    combined = jnp.sum(pair_rows.astype(jnp.float32) * weights[:, :, None], axis=1)
    layer_out = residual.astype(jnp.float32) + rms_scale(combined, specialist_branch_scale)
    return layer_out.astype(jnp.bfloat16)[None]


def solution(mesh):
    return jax.shard_map(
        shards,
        mesh=mesh,
        in_specs=(
            P("dp", "sp", None),
            P("dp", "sp", None),
            P("dp", "sp", None),
            P("dp", "sp", None),
            P("dp", "sp", None),
            P("dp", "sp", None),
            P(),
            P(None, "dp"),
            P(),
            P(),
            P(("sp", "dp"), None, None),
            P(("sp", "dp"), None, None),
            P(("sp", "dp"), None, None),
            P(),
            P("dp", "sp", None),
            P("dp", "sp", None),
        ),
        out_specs=P("dp", "sp", None),
        check_vma=False,
    )
```

```python
import jax
import jax.numpy as jnp
from jax import lax
from jax.experimental import pallas as pl
from jax.experimental.pallas import tpu as pltpu
from jax.sharding import PartitionSpec as P

D = 2048
KEY_WIDTH = 128
DV = 256
TOP = 2
BLOCK = 64


epsilon = 1e-06
softness_factor = 16.0
highest = lax.Precision.HIGHEST


def rms_scale(values, gain):
    mean_square = jnp.mean(values * values, axis=-1, keepdims=True)
    return values * lax.rsqrt(mean_square + epsilon) * gain


def local_kernel(q_ref, k_ref, v_ref, g_ref, e_ref, o_ref, r_ref, u_ref):
    rows = q_ref.shape[0]
    g = g_ref[...].astype(jnp.float32)
    logs = (jnp.minimum(g, 0.0) - jnp.log(1.0 + jnp.exp(-jnp.abs(g)))) / softness_factor
    row = lax.broadcasted_iota(jnp.int32, (rows, rows), 0)
    col = lax.broadcasted_iota(jnp.int32, (rows, rows), 1)
    causal = row >= col
    extra = jnp.sum(jnp.where(causal, e_ref[0], 0.0), axis=1, keepdims=True)
    within = extra + jnp.dot(
        causal.astype(jnp.float32), logs, precision=highest, preferred_element_type=jnp.float32
    )
    middle = within[rows // 2 - 1 : rows // 2]
    end = within[rows - 1 : rows]
    q = q_ref[...].astype(jnp.float32) * KEY_WIDTH ** (-0.5)
    k = k_ref[...].astype(jnp.float32)
    v = v_ref[...]
    lifted = (q * jnp.exp(within - middle)).astype(jnp.bfloat16)
    lowered = (k * jnp.exp(middle - within)).astype(jnp.bfloat16)
    scores = lax.dot_general(
        lifted, lowered, (((1,), (1,)), ((), ())), preferred_element_type=jnp.float32
    )
    scores = jnp.where(causal, scores, 0.0).astype(jnp.bfloat16)
    o_ref[...] = jnp.dot(scores, v, preferred_element_type=jnp.float32)
    r_ref[...] = (q * jnp.exp(within)).astype(jnp.bfloat16)
    carried = (k * jnp.exp(end - within)).astype(jnp.bfloat16)
    u_ref[0] = lax.dot_general(
        v, carried, (((0,), (0,)), ((), ())), preferred_element_type=jnp.float32
    ).astype(jnp.bfloat16)


def scan_kernel(u_ref, d_ref, s_ref):
    count = u_ref.shape[0]
    decay = jnp.exp(d_ref[0])
    state = jnp.zeros(u_ref.shape[2:], jnp.float32)
    for i in range(count):
        s_ref[i, 0] = state.astype(jnp.bfloat16)
        if i < count - 1:
            state = state * decay[i : i + 1] + u_ref[i, 0].astype(jnp.float32)


def finish_kernel(o_ref, r_ref, s_ref, gain_ref, out_ref):
    mixed = o_ref[...] + lax.dot_general(
        r_ref[...], s_ref[0], (((1,), (1,)), ((), ())), preferred_element_type=jnp.float32
    )
    out_ref[...] = rms_scale(mixed, gain_ref[...]).astype(jnp.bfloat16)


def linear_attention(query, key, value, gate, extra_shrinkage, gains):
    rows, width = query.shape
    heads = width // KEY_WIDTH
    sp_count = lax.axis_size("sp")
    own = extra_shrinkage.shape[0]
    logs = jnp.sum(jax.nn.log_sigmoid(gate.astype(jnp.float32)), axis=0) / softness_factor
    spans = jnp.transpose(extra_shrinkage.reshape(own, sp_count, rows), (1, 0, 2))
    small = jnp.concatenate([spans, logs.reshape(sp_count, own, KEY_WIDTH)], axis=2)
    small = lax.all_to_all(small, "sp", split_axis=0, concat_axis=0, tiled=True)
    extra = small[:, :, :rows].reshape(heads, 1, rows)
    decays = jnp.transpose(small[:, :, rows:] + jnp.sum(spans, axis=2)[:, :, None], (1, 0, 2))
    narrow = pl.BlockSpec((rows, KEY_WIDTH), lambda h: (0, h))
    wide = pl.BlockSpec((rows, DV), lambda h: (0, h))
    state = pl.BlockSpec((1, DV, KEY_WIDTH), lambda h: (h, 0, 0))
    inside, reached, updates = pl.pallas_call(
        local_kernel,
        grid=(heads,),
        in_specs=[narrow, narrow, wide, narrow, pl.BlockSpec((1, 1, rows), lambda h: (h, 0, 0))],
        out_specs=[wide, narrow, state],
        out_shape=[
            jax.ShapeDtypeStruct((rows, heads * DV), jnp.float32),
            jax.ShapeDtypeStruct((rows, width), jnp.bfloat16),
            jax.ShapeDtypeStruct((heads, DV, KEY_WIDTH), jnp.bfloat16),
        ],
        name="local",
    )(query, key, value, gate, extra)
    gathered = lax.all_to_all(updates, "sp", split_axis=0, concat_axis=0, tiled=True)
    stack = pl.BlockSpec((sp_count, 1, DV, KEY_WIDTH), lambda h: (0, h, 0, 0))
    entering = pl.pallas_call(
        scan_kernel,
        grid=(own,),
        in_specs=[stack, pl.BlockSpec((1, sp_count, KEY_WIDTH), lambda h: (h, 0, 0))],
        out_specs=stack,
        out_shape=jax.ShapeDtypeStruct((sp_count, own, DV, KEY_WIDTH), jnp.bfloat16),
        name="scan",
    )(gathered.reshape(sp_count, own, DV, KEY_WIDTH), decays)
    entering = lax.all_to_all(
        entering.reshape(updates.shape), "sp", split_axis=0, concat_axis=0, tiled=True
    )
    return pl.pallas_call(
        finish_kernel,
        grid=(heads,),
        in_specs=[wide, narrow, state, pl.BlockSpec((1, DV), lambda h: (0, h))],
        out_specs=wide,
        out_shape=jax.ShapeDtypeStruct((rows, heads * DV), jnp.bfloat16),
        name="finish",
    )(inside, reached, entering, gains.reshape(1, heads * DV))


PLANES = 4
LANES = 128
MESH = pl.DeviceIdType.MESH


def expert_kernel(
    out_ref, gate_hbm, up_hbm, down_hbm, ret_ref, recv, res, gate_w, up_w, down_w,
    weight_sem, send_sem, recv_sem, back_sem, ret_sem,
):
    dp_count = lax.axis_size("dp")
    total, cap, segments, lanes = out_ref.shape
    per = total // PLANES
    me = lax.axis_index("sp") * dp_count + lax.axis_index("dp")
    plane, place = me // per, lax.rem(me, per)

    def where_is(peer):
        return (peer // dp_count, lax.rem(peer, dp_count))

    weights = [
        pltpu.make_async_copy(source.at[0], target, weight_sem.at[i])
        for i, (source, target) in enumerate(
            ((gate_hbm, gate_w), (up_hbm, up_w), (down_hbm, down_w))
        )
    ]
    for copy in weights:
        copy.start()
    barrier = pltpu.get_barrier_semaphore()

    @pl.loop(1, total)
    def _(i):
        peer = lax.rem(me + i, total)
        pl.semaphore_signal(barrier, inc=1, device_id=where_is(peer), device_id_type=MESH)

    pl.semaphore_wait(barrier, total - 1)

    @pl.loop(1, total)
    def _(i):
        peer = lax.rem(plane + i, PLANES) * per + lax.rem(place + i // PLANES, per)
        pltpu.make_async_remote_copy(
            src_ref=out_ref.at[peer],
            dst_ref=recv.at[me],
            send_sem=send_sem,
            recv_sem=recv_sem.at[plane],
            device_id=where_is(peer),
            device_id_type=MESH,
        ).start()

    pltpu.make_async_copy(out_ref.at[me], recv.at[me], recv_sem.at[plane]).start()
    for copy in weights:
        copy.wait()

    @pl.loop(0, PLANES)
    def _(step):
        group = lax.rem(plane + step, PLANES)
        base = group * per
        block = recv.at[pl.ds(base, per)]
        pltpu.make_async_copy(block, block, recv_sem.at[group]).wait()
        rows = block[...].reshape(per * cap, segments * lanes)
        gate_part = jnp.dot(rows, gate_w[...], preferred_element_type=jnp.float32)
        up_part = jnp.dot(rows, up_w[...], preferred_element_type=jnp.float32)
        hidden = (jax.nn.silu(gate_part) * up_part).astype(jnp.bfloat16)
        result = jnp.dot(hidden, down_w[...], preferred_element_type=jnp.float32)
        res[pl.ds(base, per)] = result.astype(jnp.bfloat16).reshape(per, cap, segments, lanes)

        @pl.loop(0, per)
        def _(j):
            peer = base + lax.rem(place + j, per)

            @pl.when(peer != me)
            def _():
                pltpu.make_async_remote_copy(
                    src_ref=res.at[peer],
                    dst_ref=ret_ref.at[me],
                    send_sem=back_sem,
                    recv_sem=ret_sem,
                    device_id=where_is(peer),
                    device_id_type=MESH,
                ).start()

            @pl.when(peer == me)
            def _():
                pltpu.make_async_copy(res.at[me], ret_ref.at[me], ret_sem).start()

    pltpu.make_async_copy(ret_ref, ret_ref, ret_sem).wait()
    sent = out_ref.at[pl.ds(0, total - 1)]
    pltpu.make_async_copy(sent, sent, send_sem).wait()
    answered = res.at[pl.ds(0, total - 1)]
    pltpu.make_async_copy(answered, answered, back_sem).wait()


def routed_experts(outgoing, gate_weight, up_weight, down_weight):
    buffer = pltpu.VMEM(outgoing.shape, jnp.bfloat16)
    weights = [pltpu.VMEM(w.shape[1:], jnp.bfloat16) for w in (gate_weight, up_weight, down_weight)]
    vmem = pl.BlockSpec(memory_space=pltpu.VMEM)
    anywhere = pl.BlockSpec(memory_space=pl.ANY)
    row_count = outgoing.shape[0] * outgoing.shape[1]
    return pl.pallas_call(
        expert_kernel,
        in_specs=[vmem, anywhere, anywhere, anywhere],
        out_specs=vmem,
        out_shape=jax.ShapeDtypeStruct(outgoing.shape, jnp.bfloat16),
        scratch_shapes=[
            buffer,
            buffer,
            *weights,
            pltpu.SemaphoreType.DMA((3,)),
            pltpu.SemaphoreType.DMA,
            pltpu.SemaphoreType.DMA((PLANES,)),
            pltpu.SemaphoreType.DMA,
            pltpu.SemaphoreType.DMA,
        ],
        compiler_params=pltpu.CompilerParams(
            collective_id=0, has_side_effects=True, vmem_limit_bytes=56 * 1024 * 1024
        ),
        cost_estimate=pl.CostEstimate(
            flops=6 * row_count * D * gate_weight.shape[2],
            bytes_accessed=6 * D * gate_weight.shape[2],
            transcendentals=0,
        ),
        name="experts",
    )(outgoing, gate_weight, up_weight, down_weight)


def shards(
    skip_stream_entering,
    mapped_probe_matrix,
    mapped_lookup_matrix,
    mapped_content_matrix,
    retention_preactivation,
    extra_shrinkage,
    attention_group_scale,
    final_projection_matrix,
    blender_branch_scale,
    specialist_prenormal_scale,
    specialist_switch_matrix,
    specialist_expand_matrix,
    specialist_contract_matrix,
    specialist_branch_scale,
    assigned_specialists,
    dispatcher_logits,
):
    tok_rows = mapped_probe_matrix.shape[1]
    sp_count = lax.axis_size("sp")
    dp_count = lax.axis_size("dp")
    flat_heads = linear_attention(
        mapped_probe_matrix[0],
        mapped_lookup_matrix[0],
        mapped_content_matrix[0],
        retention_preactivation[0],
        extra_shrinkage[0],
        attention_group_scale,
    )
    projected = jnp.dot(
        flat_heads,
        lax.all_gather(final_projection_matrix, "dp", axis=1, tiled=True),
        preferred_element_type=jnp.float32,
    ).astype(jnp.bfloat16)
    stream = skip_stream_entering[0].astype(jnp.float32)
    residual = (stream + rms_scale(projected.astype(jnp.float32), blender_branch_scale)).astype(
        jnp.bfloat16
    )
    expert_in = rms_scale(residual.astype(jnp.float32), specialist_prenormal_scale).astype(
        jnp.bfloat16
    )
    expert_total = sp_count * dp_count
    capacity = max(2, 5 * tok_rows * TOP // (3 * expert_total))
    chosen = assigned_specialists[0].reshape(-1)
    pair_total = chosen.shape[0]
    onehot = (chosen[:, None] == jnp.arange(expert_total, dtype=jnp.int32)[None, :]).astype(
        jnp.int32
    )
    ranks = jnp.sum((jnp.cumsum(onehot, axis=0) - onehot) * onehot, axis=1)
    slots = chosen * capacity + ranks
    table = jnp.full((expert_total * capacity,), pair_total, jnp.int32)
    table = table.at[slots].set(jnp.arange(pair_total, dtype=jnp.int32))
    segments = D // LANES
    padded = jnp.concatenate([expert_in, jnp.zeros((1, D), jnp.bfloat16)], axis=0)
    padded = padded.reshape(tok_rows + 1, segments, LANES)
    outgoing = padded[table // TOP].reshape(expert_total, capacity, segments, LANES)
    returned = routed_experts(
        outgoing, specialist_switch_matrix, specialist_expand_matrix, specialist_contract_matrix
    )
    flat_back = returned.reshape(expert_total * capacity, segments, LANES)
    pair_rows = flat_back[slots].reshape(tok_rows, TOP, segments, LANES)
    weights = dispatcher_logits[0]
    weights = weights / jnp.sum(weights, axis=1, keepdims=True)
    combined = jnp.sum(pair_rows.astype(jnp.float32) * weights[:, :, None, None], axis=1)
    combined = combined.reshape(tok_rows, D)
    layer_out = residual.astype(jnp.float32) + rms_scale(combined, specialist_branch_scale)
    return layer_out.astype(jnp.bfloat16)[None]


def solution(mesh):
    return jax.shard_map(
        shards,
        mesh=mesh,
        in_specs=(
            P("dp", "sp", None),
            P("dp", "sp", None),
            P("dp", "sp", None),
            P("dp", "sp", None),
            P("dp", "sp", None),
            P("dp", "sp", None),
            P(),
            P(None, "dp"),
            P(),
            P(),
            P(("sp", "dp"), None, None),
            P(("sp", "dp"), None, None),
            P(("sp", "dp"), None, None),
            P(),
            P("dp", "sp", None),
            P("dp", "sp", None),
        ),
        out_specs=P("dp", "sp", None),
        check_vma=False,
    )
```
